32 devices in a mesh: sp: 8 (over z, x), tp: 4 (over y, core).
Axes of the slice: x: 2, y: 2, z: 4, core: 2. Of those that a mesh axis runs over, the one named last changes fastest.
Arguments:
- stream: bfloat16 [2048, 2048], P('sp'), may hold values from -6 to 6
- query: bfloat16 [2048, 1024], P('sp', 'tp'), may hold values from -6 to 6
- forget_gate_logits: bfloat16 [2048, 1024], P('sp', 'tp'), may hold values from -4 to 4
- value_input_rows: bfloat16 [2048, 1024], P('sp', 'tp'), may hold values from -6 to 6
- output_gate_logits: bfloat16 [2048, 1024], P('sp', 'tp'), may hold values from -6 to 6
- forget_floor_margin: float32 [8, 128], P('tp'), as said below
- additional_fading_speed: float32 [2048, 8], P('sp', 'tp'), may hold values from -0.7 to 0, as said below
- head_norm_gain: float32 [128], replicated, may hold values from 0.1 to 1.9
- output_head_weight: bfloat16 [1024, 2048], replicated, may hold values from -0.1875 to 0.1875
- feedforward_norm_gain: float32 [2048], replicated, may hold values from 0.1 to 1.9
- selected_expert_index: int32 [2048, 2], P('sp'), may hold values from 0 to 7, all different within a row; in each aligned block of 64 rows (0 to 63, 64 to 127, ...) at most 32 rows name the same one
- selected_expert_weight: float32 [2048, 2], P(('sp', 'tp')), may hold values from 0.2 to 1
- expert_gate_weight: bfloat16 [8, 2048, 1024], P('sp', None, 'tp'), may hold values from -0.125 to 0.125
- expert_up_weight: bfloat16 [8, 2048, 1024], P('sp', None, 'tp'), may hold values from -0.125 to 0.125
- expert_down_weight: bfloat16 [8, 1024, 2048], P('sp', 'tp'), may hold values from -0.1875 to 0.1875
Outputs:
- layer_out: bfloat16 [2048, 2048], P(('sp', 'tp'))
The draws below stay inside these ranges and needn't reach their ends.
Inputs may be any that keep to these rules, and one draw needn't show every extreme that they name: `forget_floor_margin`: positive. `additional_fading_speed`: zero at most positions. `selected_expert_index`: the 2 experts of a position differ; in each aligned block of 64 positions no expert is named more than 32 times, and in every draw some expert is named exactly 32 times in some block.
All inputs are finite; a program needn't handle non-finite values.
Results may differ from the reference program's by a relative error of at most 0.006.
Values may be sent and summed in bfloat16 or wider, within the bound.
A program may use at most 64 MiB of HBM per device.

```python
import math
import jax
import jax.numpy as jnp
import numpy as np
from jax import lax

D = 2048
SCAN_LANES = 8
HEAD_DIM = 128
FF = 1024
TOPK = 2
BLOCK = 64
TOK_DEV = 256
TOKENS = 2048
EXPERTS = 8
GROUP_ROWS = 64
CAP = 32


def draw_forget_gate_logits(key, part):
    base_key, offset_key = jax.random.split(jax.random.fold_in(key, 101))
    width = SCAN_LANES * HEAD_DIM
    base = jnp.clip(jax.random.normal(base_key, (TOKENS, width), jnp.float32), -3.0, 3.0)
    offset = jax.random.uniform(offset_key, (TOKENS // TOK_DEV, 1, SCAN_LANES, 1), jnp.float32, -1.0, 1.0)
    full = base.reshape(TOKENS // TOK_DEV, TOK_DEV, SCAN_LANES, HEAD_DIM) + offset
    return full.reshape(TOKENS, width).astype(jnp.bfloat16)


def draw_forget_floor_margin(key, part):
    order_key, fast_key, slow_key = jax.random.split(jax.random.fold_in(key, 202), 3)
    slow_count = SCAN_LANES // 2
    ranking = jax.random.permutation(order_key, SCAN_LANES)
    slow = (ranking < slow_count)[:, None]
    fast_gap = jax.random.uniform(fast_key, (SCAN_LANES, HEAD_DIM), jnp.float32, 0.04, 0.12)
    slow_gap = jax.random.uniform(slow_key, (SCAN_LANES, HEAD_DIM), jnp.float32, 0.3, 1.0) / TOKENS
    return jnp.where(slow, slow_gap, fast_gap)


def draw_additional_fading_speed(key, part):
    place_key, shift_key, depth_key = jax.random.split(jax.random.fold_in(key, 303), 3)
    first = jax.random.randint(place_key, (1, 1, SCAN_LANES), 0, TOKENS)
    shift = jax.random.randint(shift_key, (1, 1, SCAN_LANES), 1, TOKENS)
    second = (first + shift) % TOKENS
    places = jnp.concatenate([first, second], axis=0)
    depths = jax.random.uniform(depth_key, (2, 1, SCAN_LANES), jnp.float32, math.log(0.5), math.log(0.8))
    positions = jnp.arange(TOKENS, dtype=jnp.int32)[None, :, None]
    return jnp.sum(jnp.where(positions == places, depths, 0.0), axis=0)


def shard_levels(own_key, shape, cuts, smallest, high):
    loudness, own = 1.0, jax.random.fold_in(own_key, 6)
    for position, shards_of in cuts:
        heights = jnp.exp(jax.random.uniform(jax.random.fold_in(own, position), (shards_of,), jnp.float32, smallest / len(cuts), high / len(cuts)))
        loudness = loudness * jnp.repeat(heights, shape[position] // shards_of).reshape([-1 if axis == position else 1 for axis in range(len(shape))])
    return loudness


def assign_block(own_key, own, number, rows, amount, top, reach, lean):
    order = jax.random.permutation(own_key, amount)
    heavy_load, ordinary = load_shares(amount, rows * top, reach, lean, True), load_shares(amount, rows * top, reach, lean, False)
    places = jnp.arange(amount)

    def named(tallies, offset_by):
        used = int((tallies > 0).sum())
        fixed = max(1, used // 4)
        moved = fixed + (places - fixed + offset_by * (used - fixed)) % max(1, amount - fixed)
        return jnp.zeros((amount,), jnp.int32).at[order[jnp.where(places < fixed, places, moved)]].set(jnp.asarray(tallies, jnp.int32))

    tallies = jnp.where(number % 4 == 0, named(heavy_load, number // 4), named(ordinary, number - number // 4 - 1))
    mixed = jax.random.permutation(jax.random.fold_in(own, 3), amount)
    donor, taker = mixed[0:amount // 2 * 2:2], mixed[1:amount // 2 * 2:2]
    room = jnp.minimum(tallies[donor] - 1, reach - tallies[taker]) // 2
    room = jnp.where((donor == order[0]) | (taker == order[0]) | (tallies[taker] == 0), 0, jnp.maximum(room, 0))
    moved = jax.random.randint(jax.random.fold_in(own, 4), (amount // 2,), 0, 1 << 20) % (room + 1)
    tallies = tallies.at[donor].add(-moved).at[taker].add(moved)
    members = jnp.searchsorted(jnp.cumsum(tallies), jnp.arange(rows * top), side="right").astype(jnp.int32)
    grid = members.reshape(top, rows).T
    grid = grid[jax.random.permutation(jax.random.fold_in(own, 1), rows)]
    offset_by = jax.random.randint(jax.random.fold_in(own, 2), (rows, 1), 0, top)
    return jnp.take_along_axis(grid, (jnp.arange(top)[None, :] + offset_by) % top, axis=1)


def load_shares(number_of, total, bound, skew, full):
    loads = [(1 << 20) // math.isqrt(standing ** skew) + 1 for standing in range(1, number_of + 1)]
    largest = bound if full else min(bound, max(-(-total // number_of), total * loads[0] // sum(loads)))
    least = 1 if total - largest >= number_of - 1 else 0
    given, rest = [largest] + [least] * (number_of - 1), total - largest - least * (number_of - 1)
    while rest > 0:
        free = [i for i in range(1, number_of) if given[i] < largest] or [i for i in range(1, number_of) if given[i] < bound]
        pool, left = sum([loads[i] for i in free]), rest
        for i in free:
            extra = min(bound - given[i], max(1, left * loads[i] // pool), rest)
            given[i] = given[i] + extra
            rest = rest - extra
    return np.array(given)


def normal_values(own_key, extent, deviation, limit, shards=(), kind=jnp.bfloat16):
    values = deviation * jax.random.normal(own_key, extent, jnp.float32)
    if shards:
        values = values * shard_levels(own_key, extent, shards, -0.22, 0.18)
    return jnp.clip(values, -limit, limit).astype(kind)


def setup_inputs(seed: int = 0) -> dict:
    streams_of = jax.random.split(jax.random.key(seed), 16)
    stream = normal_values(streams_of[0], (TOKENS, D), 1.0, 6.0, ((0, 8),))
    query = normal_values(streams_of[1], (TOKENS, SCAN_LANES * HEAD_DIM), 1.0, 6.0, ((0, 8), (1, 4)))
    forget_gate_logits = draw_forget_gate_logits(jax.random.fold_in(streams_of[15], 71), 0)
    value_input_rows = normal_values(streams_of[3], (TOKENS, SCAN_LANES * HEAD_DIM), 1.0, 6.0, ((0, 8), (1, 4)))
    output_gate_logits = normal_values(streams_of[4], (TOKENS, SCAN_LANES * HEAD_DIM), 1.0, 6.0, ((0, 8), (1, 4)))
    forget_floor_margin = draw_forget_floor_margin(jax.random.fold_in(streams_of[15], 71), 0)
    additional_fading_speed = draw_additional_fading_speed(jax.random.fold_in(streams_of[15], 71), 0)
    head_norm_gain = jnp.clip(1.0 + 0.18 * jax.random.normal(streams_of[7], (HEAD_DIM,), jnp.float32), 0.1, 1.9)
    output_head_weight = normal_values(streams_of[8], (SCAN_LANES * HEAD_DIM, D), (SCAN_LANES * HEAD_DIM) ** -0.5, 0.1875)
    feedforward_norm_gain = jnp.clip(1.0 + 0.18 * jax.random.normal(streams_of[9], (D,), jnp.float32), 0.1, 1.9)
    selected_expert_index_keys = jax.random.split(jax.random.fold_in(streams_of[10], 1), TOKENS // GROUP_ROWS)
    selected_expert_index_turns = jax.random.permutation(jax.random.fold_in(streams_of[10], 3), TOKENS // GROUP_ROWS)
    selected_expert_index = jax.vmap(lambda own, number: assign_block(jax.random.fold_in(streams_of[10], 2), own, number, GROUP_ROWS, EXPERTS, TOPK, CAP, 1))(selected_expert_index_keys, selected_expert_index_turns).reshape((TOKENS, TOPK))
    selected_expert_weight = jnp.clip(0.2 + 0.8 * jax.random.uniform(streams_of[11], (TOKENS, TOPK), jnp.float32) ** shard_levels(streams_of[11], (TOKENS, TOPK), ((0, 32),), -0.2, 0.2), 0.2, 1.0)
    expert_gate_weight = normal_values(streams_of[12], (EXPERTS, D, FF), D ** -0.5, 0.125, ((0, 8), (2, 4)))
    expert_up_weight = normal_values(streams_of[13], (EXPERTS, D, FF), D ** -0.5, 0.125, ((0, 8), (2, 4)))
    expert_down_weight = normal_values(streams_of[14], (EXPERTS, FF, D), FF ** -0.5, 0.1875, ((0, 8), (1, 4)))
    return {"stream": stream, "query": query, "forget_gate_logits": forget_gate_logits, "value_input_rows": value_input_rows, "output_gate_logits": output_gate_logits, "forget_floor_margin": forget_floor_margin, "additional_fading_speed": additional_fading_speed, "head_norm_gain": head_norm_gain, "output_head_weight": output_head_weight, "feedforward_norm_gain": feedforward_norm_gain, "selected_expert_index": selected_expert_index, "selected_expert_weight": selected_expert_weight, "expert_gate_weight": expert_gate_weight, "expert_up_weight": expert_up_weight, "expert_down_weight": expert_down_weight}


EPS = 1e-06
HIGH = lax.Precision.HIGHEST

def cut_to_segments(array, heads):
    width = array.shape[1] // heads
    shaped = array.astype(jnp.float32).reshape(TOKENS // BLOCK, BLOCK, heads, width)
    return jnp.transpose(shaped, (0, 2, 1, 3))

def reference(stream, query, forget_gate_logits, value_input_rows, output_gate_logits, forget_floor_margin, additional_fading_speed, head_norm_gain, output_head_weight, feedforward_norm_gain, selected_expert_index, selected_expert_weight, expert_gate_weight, expert_up_weight, expert_down_weight):
    f32 = jnp.float32
    query_blk = cut_to_segments(query, SCAN_LANES)
    scores_segment_slice = cut_to_segments(forget_gate_logits, SCAN_LANES)
    value_blk = cut_to_segments(value_input_rows, SCAN_LANES)
    spike_segment_slice = cut_to_segments(additional_fading_speed, SCAN_LANES)
    clearance_amount = forget_floor_margin[None, :, None, :]
    logarithmic_fading_speed = jnp.logaddexp(jnp.log1p(-clearance_amount), jnp.log(clearance_amount) + jax.nn.log_sigmoid(scores_segment_slice)) + spike_segment_slice
    key_in = clearance_amount * jax.nn.sigmoid(-scores_segment_slice)
    causal = jnp.tril(jnp.ones((BLOCK, BLOCK), dtype=bool))[:, :, None]

    def step(state, pieces):
        query_b, key_b, value_b, log_b = pieces
        cumul = jnp.cumsum(log_b, axis=1)
        pair_log = cumul[:, :, None, :] - cumul[:, None, :, :]
        decay = jnp.exp(jnp.where(causal, pair_log, -jnp.inf))
        scores = lax.optimization_barrier(jnp.sum(query_b[:, :, None, :] * key_b[:, None, :, :] * decay, axis=-1))
        result = jnp.einsum('hts,hse->hte', scores, value_b, precision=HIGH)
        result = result + jnp.einsum('htd,hde->hte', query_b * jnp.exp(cumul), state, precision=HIGH)
        last = cumul[:, -1:, :]
        state = jnp.exp(last)[:, 0, :, None] * state + jnp.einsum('hsd,hse->hde', key_b * jnp.exp(last - cumul), value_b, precision=HIGH)
        return (state, result)
    start_state = jnp.zeros((SCAN_LANES, HEAD_DIM, HEAD_DIM), f32)
    _, recur = lax.scan(step, start_state, (query_blk, key_in, value_blk, logarithmic_fading_speed))
    recur = jnp.transpose(recur, (0, 2, 1, 3)).reshape(TOKENS, SCAN_LANES, HEAD_DIM)
    scale = lax.rsqrt(lax.optimization_barrier(jnp.mean(recur * recur, axis=-1, keepdims=True)) + EPS)
    gate_in = output_gate_logits.astype(f32).reshape(TOKENS, SCAN_LANES, HEAD_DIM)
    gated = (recur * scale * head_norm_gain * jax.nn.silu(gate_in)).astype(jnp.bfloat16).reshape(TOKENS, SCAN_LANES * HEAD_DIM)
    projected = jnp.dot(gated, output_head_weight, preferred_element_type=f32)
    mixed = (stream.astype(f32) + projected).astype(jnp.bfloat16)
    mixed_wide = lax.optimization_barrier(mixed).astype(f32)
    normed = (mixed_wide * lax.rsqrt(lax.optimization_barrier(jnp.mean(mixed_wide * mixed_wide, axis=-1, keepdims=True)) + EPS) * feedforward_norm_gain).astype(jnp.bfloat16)
    block_rows = 128
    assigned = TOKENS * TOPK
    flat_expert = selected_expert_index.reshape(-1)
    order = jnp.argsort(flat_expert, stable=True)
    sorted_expert = flat_expert[order]
    owner = order // TOPK
    counts = jnp.bincount(flat_expert, length=EXPERTS)
    padded_counts = (counts + block_rows - 1) // block_rows * block_rows
    padded_end = jnp.cumsum(padded_counts)
    padded_start = padded_end - padded_counts
    first = jnp.cumsum(counts) - counts
    dest = padded_start[sorted_expert] + jnp.arange(assigned, dtype=jnp.int32) - first[sorted_expert]
    block_count = -(-assigned // block_rows) + EXPERTS
    buffer = jnp.zeros((block_count * block_rows, D), jnp.bfloat16).at[dest].set(normed[owner])
    block_expert = jnp.minimum(jnp.searchsorted(padded_end, jnp.arange(block_count) * block_rows, side='right'), EXPERTS - 1).astype(jnp.int32)

    def expert_block(pieces):
        rows, expert = pieces
        gate_part = jnp.dot(rows, expert_gate_weight[expert], preferred_element_type=f32)
        up_part = jnp.dot(rows, expert_up_weight[expert], preferred_element_type=f32)
        hidden = (jax.nn.silu(gate_part) * up_part).astype(jnp.bfloat16)
        return jnp.dot(hidden, expert_down_weight[expert], preferred_element_type=f32).astype(jnp.bfloat16)
    outputs = lax.map(expert_block, (buffer.reshape(block_count, block_rows, D), block_expert)).reshape(-1, D)
    weighted = outputs[dest].astype(f32) * selected_expert_weight.reshape(-1)[order][:, None]
    routed = jax.ops.segment_sum(weighted, owner, num_segments=TOKENS)
    return (mixed_wide + routed).astype(jnp.bfloat16)
```

```python
import functools

import jax
import jax.numpy as jnp
from jax import lax
from jax.experimental import pallas as pl
from jax.experimental.pallas import tpu as pltpu
from jax.sharding import PartitionSpec as P

BLOCK = 64


EPS = 1e-06
HIGH = lax.Precision.HIGHEST
MESH = pl.DeviceIdType.MESH
VMEM_LIMIT = 60 * 1024 * 1024


def xor(a, b, size):
    total, bit = 0, 1
    while bit < size:
        total = total + lax.rem(lax.div(a, jnp.int32(bit)) + lax.div(jnp.int32(b), jnp.int32(bit)), jnp.int32(2)) * bit
        bit *= 2
    return total


def loop(lo, hi, body):
    lax.fori_loop(lo, hi, lambda i, c: (body(i), c)[1], 0)


def carry_kernel(n, state_ref, decay_ref, out_ref, send, states, decays, ss, rs, ds, dr):
    s, t = lax.axis_index("sp"), lax.axis_index("tp")
    barrier = pltpu.get_barrier_semaphore()
    loop(1, n, lambda k: pl.semaphore_signal(barrier, inc=1, device_id=(lax.rem(s + k, n), t), device_id_type=MESH))
    send[...] = state_ref[...].astype(jnp.bfloat16)
    pl.semaphore_wait(barrier, n - 1)

    def copies(k, source, target):
        a = pltpu.make_async_remote_copy(
            src_ref=send, dst_ref=states.at[source], send_sem=ss.at[k], recv_sem=rs.at[k],
            device_id=(target, t), device_id_type=MESH)
        b = pltpu.make_async_remote_copy(
            src_ref=decay_ref, dst_ref=decays.at[source], send_sem=ds.at[k], recv_sem=dr.at[k],
            device_id=(target, t), device_id_type=MESH)
        return a, b

    def start(k):
        @pl.when(s + k < n)
        def _():
            for c in copies(k, s, s + k):
                c.start()

    loop(1, n, start)

    def arrive(k):
        @pl.when(s >= k)
        def _():
            for c in copies(k, s - k, s - k):
                c.wait_recv()

    loop(1, n, arrive)
    out_ref[...] = jnp.zeros_like(out_ref)

    def fold(j):
        @pl.when(j < s)
        def _():
            out_ref[...] = out_ref[...] * decays[j][:, None, :] + states[j].astype(jnp.float32)

    loop(0, n, fold)

    def sent(k):
        @pl.when(s + k < n)
        def _():
            for c in copies(k, s, s + k):
                c.wait_send()

    loop(1, n, sent)


def carry_in(n, state, decay):
    lanes, width = decay.shape
    return pl.pallas_call(
        functools.partial(carry_kernel, n),
        out_shape=jax.ShapeDtypeStruct(state.shape, jnp.float32),
        in_specs=[pl.BlockSpec(memory_space=pltpu.VMEM)] * 2,
        out_specs=pl.BlockSpec(memory_space=pltpu.VMEM),
        scratch_shapes=[
            pltpu.VMEM(state.shape, jnp.bfloat16),
            pltpu.VMEM((n,) + state.shape, jnp.bfloat16),
            pltpu.VMEM((n,) + decay.shape, jnp.float32),
        ] + [pltpu.SemaphoreType.DMA((n,))] * 4,
        compiler_params=pltpu.CompilerParams(collective_id=0, has_side_effects=True, vmem_limit_bytes=VMEM_LIMIT),
        name="carry_in",
    )(state, decay)


def expert_kernel(
    n, tps, rows, cap,
    gated_ref, stream_ref, gain_ref, place_ref, whi_ref, wlo_ref, wo_hbm, wg_hbm, wu_hbm, wd_hbm,
    out_ref,
    gbuf, wo, wg, wu, wd, mixed, normed, outgoing, arr, part, keep, keep2, rb1, sb2, rb2, back, ret,
    wsem, gs, gr, ds, dr, ys, yr, cs, cr, s1s, s1r, s2s, s2r, bs, br,
):
    f32, bf16 = jnp.float32, jnp.bfloat16
    s, t = lax.axis_index("sp"), lax.axis_index("tp")
    ty, tc = lax.div(t, jnp.int32(2)), lax.rem(t, jnp.int32(2))
    far, near = t + 2 - 4 * ty, t + 1 - 2 * tc
    mine, pair, other_pair = tc * 2 + ty, tc * 2, 2 - tc * 2
    width = stream_ref.shape[1]
    cw = gbuf.shape[2]
    loads = [pltpu.make_async_copy(a, b, wsem.at[i]) for i, (a, b) in enumerate(
        ((wo_hbm, wo), (wg_hbm, wg), (wu_hbm, wu), (wd_hbm, wd)))]
    for c in loads:
        c.start()
    barrier = pltpu.get_barrier_semaphore()
    loop(1, n, lambda k: pl.semaphore_signal(barrier, inc=1, device_id=(xor(s, k, n), t), device_id_type=MESH))
    for j in range(1, tps):
        pl.semaphore_signal(barrier, inc=1, device_id=(s, xor(t, j, tps)), device_id_type=MESH)
    pl.semaphore_wait(barrier, n - 1 + tps - 1)

    def remote(src, dst, send, recv, device):
        return pltpu.make_async_remote_copy(
            src_ref=src, dst_ref=dst, send_sem=send, recv_sem=recv, device_id=device, device_id_type=MESH)

    def g_copy(j):
        q = xor(t, j, tps)
        return remote(gated_ref.at[q], gbuf.at[t], gs.at[j], gr.at[j], (s, q))

    for j in range(1, tps):
        g_copy(j).start()
    gbuf[t] = gated_ref[t]
    loads[0].wait()
    for j in range(1, tps):
        g_copy(j).wait_recv()

    step = min(512, width)
    square = jnp.zeros((rows, 1), f32)
    for c in range(0, width, step):
        total = stream_ref[:, c:c + step].astype(f32)
        acc = jnp.zeros((rows, step), f32)
        for q in range(tps):
            acc = acc + jnp.dot(gbuf[q], wo[q * cw:(q + 1) * cw, c:c + step], preferred_element_type=f32)
        rounded = (total + acc).astype(bf16)
        mixed[:, c:c + step] = rounded
        wide = rounded.astype(f32)
        square = square + jnp.sum(wide * wide, axis=-1, keepdims=True)
    scale = lax.rsqrt(square / width + EPS)
    for c in range(0, width, step):
        normed[:, c:c + step] = (mixed[:, c:c + step].astype(f32) * scale * gain_ref[:, c:c + step]).astype(bf16)

    def d_copy(k):
        return remote(outgoing.at[k], arr.at[k, mine], ds.at[k], dr.at[k], (xor(s, k, n), t))

    def y_copy(k):
        return remote(arr.at[k, mine], arr.at[k, mine], ys.at[k], yr.at[k], (s, far))

    def c_copy(k):
        held = arr.at[k, pl.ds(pair, 2)]
        return remote(held, held, cs.at[k], cr.at[k], (s, near))

    def s1_copy(k):
        return remote(arr.at[k, pl.ds(other_pair, 2)], rb1.at[k], s1s.at[k], s1r.at[k], (s, near))

    def s2_copy(k):
        return remote(sb2.at[k], rb2.at[k], s2s.at[k], s2r.at[k], (s, far))

    def b_copy(k):
        return remote(back.at[k], ret.at[s], bs.at[k], br.at[k], (xor(s, k, n), t))

    def dispatch(k):
        block = jnp.dot(place_ref[xor(s, k, n)], normed[...], preferred_element_type=f32).astype(bf16)
        outgoing[k] = block
        d_copy(k).start()

    arr[0, mine] = jnp.dot(place_ref[s], normed[...], preferred_element_type=f32).astype(bf16)
    loop(1, n, dispatch)
    for c in loads[1:]:
        c.wait()

    def turn(i):
        @pl.when(i < n)
        def _():
            @pl.when(i > 0)
            def _():
                d_copy(i).wait_recv()
            y_copy(i).start()

        b = i - 1
        @pl.when((b >= 0) & (b < n))
        def _():
            y_copy(b).wait_recv()
            c_copy(b).start()

        e = i - 4
        @pl.when((e >= 0) & (e < n))
        def _():
            s2_copy(e).wait_recv()
            done = (keep2[lax.rem(e, jnp.int32(2))] + rb2[e].astype(f32)).astype(bf16)

            @pl.when(e == 0)
            def _():
                ret[s] = done

            @pl.when(e > 0)
            def _():
                back[e] = done
                b_copy(e).start()

        d = i - 3
        @pl.when((d >= 0) & (d < n))
        def _():
            s1_copy(d).wait_recv()
            slot = lax.rem(d, jnp.int32(2))
            sb2[d] = (keep[slot, 1 - ty] + rb1[d, 1 - ty].astype(f32)).astype(bf16)
            s2_copy(d).start()
            keep2[slot] = keep[slot, ty] + rb1[d, ty].astype(f32)

        c = i - 2
        @pl.when((c >= 0) & (c < n))
        def _():
            c_copy(c).wait_recv()
            x = arr[c].reshape(tps * cap, width)
            gate = jnp.dot(x, wg[...], preferred_element_type=f32)
            up = jnp.dot(x, wu[...], preferred_element_type=f32)
            hidden = (gate * jax.nn.sigmoid(gate) * up).astype(bf16)
            for k in range(0, width, step):
                piece = jnp.dot(hidden, wd[:, k:k + step], preferred_element_type=f32)
                part[:, :, k:k + step] = piece.reshape(tps, cap, step)
            arr[c, pl.ds(other_pair, 2)] = part[pl.ds(other_pair, 2)].astype(bf16)
            s1_copy(c).start()
            keep[lax.rem(c, jnp.int32(2))] = part[pl.ds(pair, 2)]

    loop(0, n + 4, turn)

    def arrived(k):
        b_copy(k).wait_recv()

    loop(1, n, arrived)
    for c in range(0, width, step):
        held = ret[:, :, c:c + step].reshape(n * cap, step)
        routed = jnp.dot(whi_ref[...], held, preferred_element_type=f32)
        routed = routed + jnp.dot(wlo_ref[...], held, preferred_element_type=f32)
        out_ref[:, c:c + step] = (mixed[:, c:c + step].astype(f32) + routed).astype(bf16)

    for j in range(1, tps):
        g_copy(j).wait_send()

    def sent(k):
        y_copy(k).wait_send()
        c_copy(k).wait_send()
        s1_copy(k).wait_send()
        s2_copy(k).wait_send()

        @pl.when(k > 0)
        def _():
            d_copy(k).wait_send()
            b_copy(k).wait_send()

    loop(0, n, sent)


def experts_of(n, tps, cap, gated, stream, gain, place, whi, wlo, w_out, w_gate, w_up, w_down):
    rows, width = stream.shape
    bf16, f32 = jnp.bfloat16, jnp.float32
    vmem = pl.BlockSpec(memory_space=pltpu.VMEM)
    hbm = pl.BlockSpec(memory_space=pl.ANY)
    block = (cap, width)
    sem = pltpu.SemaphoreType.DMA
    return pl.pallas_call(
        functools.partial(expert_kernel, n, tps, rows, cap),
        out_shape=jax.ShapeDtypeStruct((rows, width), bf16),
        in_specs=[vmem] * 6 + [hbm] * 4,
        out_specs=vmem,
        scratch_shapes=[
            pltpu.VMEM(gated.shape, bf16),
            pltpu.VMEM(w_out.shape, bf16),
            pltpu.VMEM(w_gate.shape, bf16),
            pltpu.VMEM(w_up.shape, bf16),
            pltpu.VMEM(w_down.shape, bf16),
            pltpu.VMEM((rows, width), bf16),
            pltpu.VMEM((rows, width), bf16),
            pltpu.VMEM((n,) + block, bf16),
            pltpu.VMEM((n, tps) + block, bf16),
            pltpu.VMEM((tps,) + block, f32),
            pltpu.VMEM((2, 2) + block, f32),
            pltpu.VMEM((2,) + block, f32),
            pltpu.VMEM((n, 2) + block, bf16),
            pltpu.VMEM((n,) + block, bf16),
            pltpu.VMEM((n,) + block, bf16),
            pltpu.VMEM((n,) + block, bf16),
            pltpu.VMEM((n,) + block, bf16),
            sem((4,)), sem((tps,)), sem((tps,)),
        ] + [sem((n,))] * 12,
        compiler_params=pltpu.CompilerParams(collective_id=1, has_side_effects=True, vmem_limit_bytes=VMEM_LIMIT),
        name="experts",
    )(gated, stream, gain, place, whi, wlo, w_out, w_gate, w_up, w_down)


def cut_to_segments(array, segment_span, heads):
    width = array.shape[1] // heads
    shaped = array.astype(jnp.float32).reshape(
        array.shape[0] // segment_span, segment_span, heads, width
    )
    return jnp.transpose(shaped, (0, 2, 1, 3))


def slot_ranks(chosen, experts):
    onehot = (chosen[:, :, None] == jnp.arange(experts, dtype=jnp.int32)[None, None, :]).astype(
        jnp.int32
    )
    earlier = jnp.cumsum(onehot, axis=1) - onehot
    return jnp.sum(earlier * onehot, axis=2)


def per_device(
    stream,
    query,
    forget_gate_logits,
    value_input_rows,
    output_gate_logits,
    forget_floor_margin,
    additional_fading_speed,
    head_norm_gain,
    output_head_weight,
    feedforward_norm_gain,
    selected_expert_index,
    selected_expert_weight,
    expert_gate_weight,
    expert_up_weight,
    expert_down_weight,
):
    f32 = jnp.float32
    tok_rows, model_width = stream.shape
    local_scan_lanes, head_dim = forget_floor_margin.shape
    segment_span = BLOCK
    tp_count = lax.axis_size("tp")
    tp_rank = lax.axis_index("tp")
    query_blk = cut_to_segments(query, segment_span, local_scan_lanes)
    scores_segment_slice = cut_to_segments(forget_gate_logits, segment_span, local_scan_lanes)
    value_blk = cut_to_segments(value_input_rows, segment_span, local_scan_lanes)
    spike_segment_slice = cut_to_segments(additional_fading_speed, segment_span, local_scan_lanes)
    clearance_amount = forget_floor_margin[None, :, None, :]
    logarithmic_fading_speed = (
        jnp.logaddexp(
            jnp.log1p(-clearance_amount),
            jnp.log(clearance_amount) + jax.nn.log_sigmoid(scores_segment_slice),
        )
        + spike_segment_slice
    )
    key_in = clearance_amount * jax.nn.sigmoid(-scores_segment_slice)
    cumul = jnp.cumsum(logarithmic_fading_speed, axis=2)
    last = cumul[:, :, -1:, :]
    causal = jnp.tril(jnp.ones((segment_span, segment_span), dtype=bool))[:, :, None]
    pair_log = cumul[:, :, :, None, :] - cumul[:, :, None, :, :]
    decay = jnp.exp(jnp.where(causal, pair_log, -jnp.inf))
    scores = jnp.sum(query_blk[:, :, :, None, :] * key_in[:, :, None, :, :] * decay, axis=-1)
    inner = jnp.einsum("bhts,bhse->bhte", scores, value_blk, precision=HIGH)
    block_state = jnp.einsum(
        "bhsd,bhse->bhed", key_in * jnp.exp(last - cumul), value_blk, precision=HIGH
    )
    block_last = last[:, :, 0, :]
    last_cumul = jnp.cumsum(block_last, axis=0)
    device_decay = jnp.exp(last_cumul[-1])
    suffix = jnp.exp(last_cumul[-1][None] - last_cumul)
    local_final = jnp.sum(suffix[:, :, None, :] * block_state, axis=0)
    n = lax.axis_size("sp")
    incoming = carry_in(n, local_final, device_decay)
    chain_starts = []
    for blk in range(block_state.shape[0]):
        chain_starts.append(incoming)
        incoming = jnp.exp(block_last[blk])[:, None, :] * incoming + block_state[blk]
    recur = inner + jnp.einsum(
        "bhtd,bhed->bhte", query_blk * jnp.exp(cumul), jnp.stack(chain_starts), precision=HIGH
    )
    recur = jnp.transpose(recur, (0, 2, 1, 3)).reshape(tok_rows, local_scan_lanes, head_dim)
    scale = lax.rsqrt(jnp.mean(recur * recur, axis=-1, keepdims=True) + EPS)
    gate_in = output_gate_logits.astype(f32).reshape(tok_rows, local_scan_lanes, head_dim)
    gated = (
        (recur * scale * head_norm_gain * jax.nn.silu(gate_in))
        .astype(jnp.bfloat16)
        .reshape(tok_rows, local_scan_lanes * head_dim)
    )
    topk = selected_expert_index.shape[1]
    experts = n * expert_gate_weight.shape[0]
    group_rows = tok_rows // tp_count
    cap = 2 * topk * group_rows // experts
    cap = -(-cap // 16) * 16
    own_route = lax.dynamic_slice_in_dim(selected_expert_index, tp_rank * group_rows, group_rows, 0)
    own_stream = lax.dynamic_slice_in_dim(stream, tp_rank * group_rows, group_rows, 0)
    own_ranks = slot_ranks(own_route.reshape(1, -1), experts)[0].reshape(group_rows, topk)
    slot = own_route * cap + own_ranks
    slots = jnp.arange(experts * cap, dtype=jnp.int32)
    place = jnp.zeros((experts * cap, group_rows), f32)
    weight = jnp.zeros((group_rows, experts * cap), f32)
    for j in range(topk):
        place = place + (slot[:, j][None, :] == slots[:, None]).astype(f32)
        weight = weight + jnp.where(
            slot[:, j][:, None] == slots[None, :], selected_expert_weight[:, j][:, None], 0.0
        )
    place = place.astype(jnp.bfloat16).reshape(experts, cap, group_rows)
    weight_high = lax.reduce_precision(weight, 8, 7)
    weight_low = (weight - weight_high).astype(jnp.bfloat16)
    return experts_of(
        n,
        tp_count,
        cap,
        gated.reshape(tp_count, group_rows, local_scan_lanes * head_dim),
        own_stream,
        feedforward_norm_gain[None, :],
        place,
        weight_high.astype(jnp.bfloat16),
        weight_low,
        output_head_weight,
        expert_gate_weight[0],
        expert_up_weight[0],
        expert_down_weight[0],
    )


def solution(mesh):
    return jax.shard_map(
        per_device,
        mesh=mesh,
        in_specs=(
            P("sp", None),
            P("sp", "tp"),
            P("sp", "tp"),
            P("sp", "tp"),
            P("sp", "tp"),
            P("tp", None),
            P("sp", "tp"),
            P(),
            P(),
            P(),
            P("sp", None),
            P(("sp", "tp"), None),
            P("sp", None, "tp"),
            P("sp", None, "tp"),
            P("sp", "tp", None),
        ),
        out_specs=P(("sp", "tp"), None),
        check_vma=False,
    )
```

```python
import functools

import jax
import jax.numpy as jnp
from jax import lax
from jax.experimental import pallas as pl
from jax.experimental.pallas import tpu as pltpu
from jax.sharding import PartitionSpec as P

BLOCK = 64
SUB = 16


EPS = 1e-06
HIGH = lax.Precision.HIGHEST
MESH = pl.DeviceIdType.MESH
VMEM_LIMIT = 60 * 1024 * 1024


def xor(a, b, size):
    total, bit = 0, 1
    while bit < size:
        total = total + lax.rem(lax.div(a, jnp.int32(bit)) + lax.div(jnp.int32(b), jnp.int32(bit)), jnp.int32(2)) * bit
        bit *= 2
    return total


def loop(lo, hi, body):
    lax.fori_loop(lo, hi, lambda i, c: (body(i), c)[1], 0)


def wide_dot(a, b, contract):
    return lax.dot_general(a, b, ((contract[:1], contract[1:]), ((), ())), precision=HIGH, preferred_element_type=jnp.float32)


def scan_kernel(
    n, lanes, dim, query_ref, logit_ref, value_ref, gate_ref, margin_ref, fade_ref, gain_ref, out_ref,
    cum, key, rec, chain, send, decay, carried, states, decays, ss, rs, ds, dr,
):
    f32, bf16 = jnp.float32, jnp.bfloat16
    s, t = lax.axis_index("sp"), lax.axis_index("tp")
    rows = query_ref.shape[0]
    count = rows // BLOCK
    barrier = pltpu.get_barrier_semaphore()
    loop(1, n, lambda k: pl.semaphore_signal(barrier, inc=1, device_id=(lax.rem(s + k, n), t), device_id_type=MESH))
    heads = [slice(h * dim, (h + 1) * dim) for h in range(lanes)]
    row = lax.broadcasted_iota(jnp.int32, (BLOCK, BLOCK), 0)
    lower = (row >= lax.broadcasted_iota(jnp.int32, (BLOCK, BLOCK), 1)).astype(f32)
    for h, sl in enumerate(heads):
        entering_key = margin_ref[h:h + 1, :] * jax.nn.sigmoid(-logit_ref[:, sl].astype(f32))
        key[:, sl] = entering_key
        rec[:, sl] = jnp.log1p(-entering_key) + fade_ref[:, h:h + 1]
    for b in range(count):
        part = slice(b * BLOCK, (b + 1) * BLOCK)
        cum[part, :] = wide_dot(lower, rec[part, :], (1, 0))
    offsets = [jnp.zeros((1, lanes * dim), f32)]
    for b in range(count):
        offsets.append(offsets[-1] + cum[(b + 1) * BLOCK - 1:(b + 1) * BLOCK, :])
    for b in range(count):
        part = slice(b * BLOCK, (b + 1) * BLOCK)
        rec[part, :] = key[part, :] * jnp.exp(offsets[-1] - offsets[b] - cum[part, :])
    for h, sl in enumerate(heads):
        send[h] = wide_dot(value_ref[:, sl].astype(f32), rec[:, sl], (0, 0)).astype(bf16)
        decay[h:h + 1, :] = jnp.exp(offsets[-1][:, sl])
    pl.semaphore_wait(barrier, n - 1)

    def copies(k, source, target):
        a = pltpu.make_async_remote_copy(
            src_ref=send, dst_ref=states.at[source], send_sem=ss.at[k], recv_sem=rs.at[k],
            device_id=(target, t), device_id_type=MESH)
        b = pltpu.make_async_remote_copy(
            src_ref=decay, dst_ref=decays.at[source], send_sem=ds.at[k], recv_sem=dr.at[k],
            device_id=(target, t), device_id_type=MESH)
        return a, b

    def start(k):
        @pl.when(s + k < n)
        def _():
            for c in copies(k, s, s + k):
                c.start()

    loop(1, n, start)
    chain[...] = jnp.zeros_like(chain)
    near = lax.broadcasted_iota(jnp.int32, (BLOCK // SUB, SUB, 1), 1)
    below = lax.broadcasted_iota(jnp.int32, (BLOCK, 1), 0)

    def inside(b):
        part = pl.ds(pl.multiple_of(b * BLOCK, BLOCK), BLOCK)
        for h, sl in enumerate(heads):
            q, v = query_ref[part, sl].astype(f32), value_ref[part, sl].astype(f32)
            c, k = cum[part, sl], key[part, sl]
            cut = (BLOCK // SUB, SUB, dim)
            q3, v3, c3, k3 = q.reshape(cut), v.reshape(cut), c.reshape(cut), k.reshape(cut)
            inner = jnp.zeros(cut, f32)
            for j in range(SUB):
                fade = jnp.exp(jnp.minimum(c3 - c3[:, j:j + 1, :], 0.0))
                score = jnp.sum(q3 * fade * k3[:, j:j + 1, :], axis=-1, keepdims=True)
                inner = inner + jnp.where(near >= j, score, 0.0) * v3[:, j:j + 1, :]
            scores = [jnp.zeros((SUB, BLOCK), f32)]
            for i in range(SUB, BLOCK, SUB):
                edge = c[i - 1:i, :]
                older = jnp.where(below < i, k * jnp.exp(jnp.minimum(edge - c, 0.0)), 0.0)
                scores.append(wide_dot(q[i:i + SUB] * jnp.exp(c[i:i + SUB] - edge), older, (1, 1)))
            last = c[BLOCK - 1:BLOCK, :]
            rec[part, sl] = (
                inner.reshape(BLOCK, dim)
                + wide_dot(jnp.concatenate(scores, axis=0), v, (1, 0))
                + wide_dot(q * jnp.exp(c), chain[h], (1, 1))
            )
            chain[h] = jnp.exp(last) * chain[h] + wide_dot(v, k * jnp.exp(last - c), (0, 0))

    loop(0, count, inside)

    def arrive(k):
        @pl.when(s >= k)
        def _():
            for c in copies(k, s - k, s - k):
                c.wait_recv()

    loop(1, n, arrive)
    carried[...] = jnp.zeros_like(carried)

    def fold(j):
        @pl.when(j < s)
        def _():
            for h in range(lanes):
                carried[h] = carried[h] * decays[j, h:h + 1, :] + states[j, h].astype(f32)

    loop(0, n, fold)
    for b in range(count):
        part = slice(b * BLOCK, (b + 1) * BLOCK)
        cum[part, :] = jnp.exp(cum[part, :] + offsets[b])
    for h, sl in enumerate(heads):
        recur = rec[:, sl] + wide_dot(query_ref[:, sl].astype(f32) * cum[:, sl], carried[h], (1, 1))
        scale = lax.rsqrt(jnp.mean(recur * recur, axis=-1, keepdims=True) + EPS)
        gate = gate_ref[:, sl].astype(f32)
        out_ref[:, sl] = (recur * scale * gain_ref[...] * (gate * jax.nn.sigmoid(gate))).astype(bf16)

    def sent(k):
        @pl.when(s + k < n)
        def _():
            for c in copies(k, s, s + k):
                c.wait_send()

    loop(1, n, sent)


def gated_scan(n, query, logits, value, gate, margin, fade, gain):
    lanes, dim = margin.shape
    f32, bf16 = jnp.float32, jnp.bfloat16
    state = (lanes, dim, dim)
    return pl.pallas_call(
        functools.partial(scan_kernel, n, lanes, dim),
        out_shape=jax.ShapeDtypeStruct(query.shape, bf16),
        in_specs=[pl.BlockSpec(memory_space=pltpu.VMEM)] * 7,
        out_specs=pl.BlockSpec(memory_space=pltpu.VMEM),
        scratch_shapes=[
            pltpu.VMEM(query.shape, f32),
            pltpu.VMEM(query.shape, f32),
            pltpu.VMEM(query.shape, f32),
            pltpu.VMEM(state, f32),
            pltpu.VMEM(state, bf16),
            pltpu.VMEM((lanes, dim), f32),
            pltpu.VMEM(state, f32),
            pltpu.VMEM((n,) + state, bf16),
            pltpu.VMEM((n, lanes, dim), f32),
        ] + [pltpu.SemaphoreType.DMA((n,))] * 4,
        compiler_params=pltpu.CompilerParams(collective_id=0, has_side_effects=True, vmem_limit_bytes=VMEM_LIMIT),
        name="gated_scan",
    )(query, logits, value, gate, margin, fade, gain)


def expert_kernel(
    n, tps, rows, cap,
    gated_ref, stream_ref, gain_ref, place_ref, whi_ref, wlo_ref, wo_hbm, wg_hbm, wu_hbm, wd_hbm,
    out_ref,
    gbuf, wo, wg, wu, wd, mixed, normed, outgoing, arr, part, keep, keep2, rb1, sb2, rb2, back, ret,
    wsem, gs, gr, ds, dr, ys, yr, cs, cr, s1s, s1r, s2s, s2r, bs, br,
):
    f32, bf16 = jnp.float32, jnp.bfloat16
    s, t = lax.axis_index("sp"), lax.axis_index("tp")
    ty, tc = lax.div(t, jnp.int32(2)), lax.rem(t, jnp.int32(2))
    far, near = t + 2 - 4 * ty, t + 1 - 2 * tc
    mine, pair, other_pair = tc * 2 + ty, tc * 2, 2 - tc * 2
    width = stream_ref.shape[1]
    cw = gbuf.shape[2]
    loads = [pltpu.make_async_copy(a, b, wsem.at[i]) for i, (a, b) in enumerate(
        ((wo_hbm, wo), (wg_hbm, wg), (wu_hbm, wu), (wd_hbm, wd)))]
    for c in loads:
        c.start()
    barrier = pltpu.get_barrier_semaphore()
    loop(1, n, lambda k: pl.semaphore_signal(barrier, inc=1, device_id=(xor(s, k, n), t), device_id_type=MESH))
    for j in range(1, tps):
        pl.semaphore_signal(barrier, inc=1, device_id=(s, xor(t, j, tps)), device_id_type=MESH)
    pl.semaphore_wait(barrier, n - 1 + tps - 1)

    def remote(src, dst, send, recv, device):
        return pltpu.make_async_remote_copy(
            src_ref=src, dst_ref=dst, send_sem=send, recv_sem=recv, device_id=device, device_id_type=MESH)

    def g_copy(j):
        q = xor(t, j, tps)
        return remote(gated_ref.at[q], gbuf.at[t], gs.at[j], gr.at[j], (s, q))

    for j in range(1, tps):
        g_copy(j).start()
    gbuf[t] = gated_ref[t]
    loads[0].wait()
    for j in range(1, tps):
        g_copy(j).wait_recv()

    step = min(512, width)
    square = jnp.zeros((rows, 1), f32)
    for c in range(0, width, step):
        total = stream_ref[:, c:c + step].astype(f32)
        acc = jnp.zeros((rows, step), f32)
        for q in range(tps):
            acc = acc + jnp.dot(gbuf[q], wo[q * cw:(q + 1) * cw, c:c + step], preferred_element_type=f32)
        rounded = (total + acc).astype(bf16)
        mixed[:, c:c + step] = rounded
        wide = rounded.astype(f32)
        square = square + jnp.sum(wide * wide, axis=-1, keepdims=True)
    scale = lax.rsqrt(square / width + EPS)
    for c in range(0, width, step):
        normed[:, c:c + step] = (mixed[:, c:c + step].astype(f32) * scale * gain_ref[:, c:c + step]).astype(bf16)

    def d_copy(k):
        return remote(outgoing.at[k], arr.at[k, mine], ds.at[k], dr.at[k], (xor(s, k, n), t))

    def y_copy(k):
        return remote(arr.at[k, mine], arr.at[k, mine], ys.at[k], yr.at[k], (s, far))

    def c_copy(k):
        held = arr.at[k, pl.ds(pair, 2)]
        return remote(held, held, cs.at[k], cr.at[k], (s, near))

    def s1_copy(k):
        return remote(arr.at[k, pl.ds(other_pair, 2)], rb1.at[k], s1s.at[k], s1r.at[k], (s, near))

    def s2_copy(k):
        return remote(sb2.at[k], rb2.at[k], s2s.at[k], s2r.at[k], (s, far))

    def b_copy(k):
        return remote(back.at[k], ret.at[s], bs.at[k], br.at[k], (xor(s, k, n), t))

    def dispatch(k):
        block = jnp.dot(place_ref[xor(s, k, n)], normed[...], preferred_element_type=f32).astype(bf16)
        outgoing[k] = block
        d_copy(k).start()

    arr[0, mine] = jnp.dot(place_ref[s], normed[...], preferred_element_type=f32).astype(bf16)
    loop(1, n, dispatch)
    for c in loads[1:]:
        c.wait()

    def turn(i):
        @pl.when(i < n)
        def _():
            @pl.when(i > 0)
            def _():
                d_copy(i).wait_recv()
            y_copy(i).start()

        b = i - 1
        @pl.when((b >= 0) & (b < n))
        def _():
            y_copy(b).wait_recv()
            c_copy(b).start()

        e = i - 4
        @pl.when((e >= 0) & (e < n))
        def _():
            s2_copy(e).wait_recv()
            done = (keep2[lax.rem(e, jnp.int32(2))] + rb2[e].astype(f32)).astype(bf16)

            @pl.when(e == 0)
            def _():
                ret[s] = done

            @pl.when(e > 0)
            def _():
                back[e] = done
                b_copy(e).start()

        d = i - 3
        @pl.when((d >= 0) & (d < n))
        def _():
            s1_copy(d).wait_recv()
            slot = lax.rem(d, jnp.int32(2))
            sb2[d] = (keep[slot, 1 - ty] + rb1[d, 1 - ty].astype(f32)).astype(bf16)
            s2_copy(d).start()
            keep2[slot] = keep[slot, ty] + rb1[d, ty].astype(f32)

        c = i - 2
        @pl.when((c >= 0) & (c < n))
        def _():
            c_copy(c).wait_recv()
            x = arr[c].reshape(tps * cap, width)
            gate = jnp.dot(x, wg[...], preferred_element_type=f32)
            up = jnp.dot(x, wu[...], preferred_element_type=f32)
            hidden = (gate * jax.nn.sigmoid(gate) * up).astype(bf16)
            for k in range(0, width, step):
                piece = jnp.dot(hidden, wd[:, k:k + step], preferred_element_type=f32)
                part[:, :, k:k + step] = piece.reshape(tps, cap, step)
            arr[c, pl.ds(other_pair, 2)] = part[pl.ds(other_pair, 2)].astype(bf16)
            s1_copy(c).start()
            keep[lax.rem(c, jnp.int32(2))] = part[pl.ds(pair, 2)]

    loop(0, n + 4, turn)

    def arrived(k):
        b_copy(k).wait_recv()

    loop(1, n, arrived)
    for c in range(0, width, step):
        held = ret[:, :, c:c + step].reshape(n * cap, step)
        routed = jnp.dot(whi_ref[...], held, preferred_element_type=f32)
        routed = routed + jnp.dot(wlo_ref[...], held, preferred_element_type=f32)
        out_ref[:, c:c + step] = (mixed[:, c:c + step].astype(f32) + routed).astype(bf16)

    for j in range(1, tps):
        g_copy(j).wait_send()

    def sent(k):
        y_copy(k).wait_send()
        c_copy(k).wait_send()
        s1_copy(k).wait_send()
        s2_copy(k).wait_send()

        @pl.when(k > 0)
        def _():
            d_copy(k).wait_send()
            b_copy(k).wait_send()

    loop(0, n, sent)


def experts_of(n, tps, cap, gated, stream, gain, place, whi, wlo, w_out, w_gate, w_up, w_down):
    rows, width = stream.shape
    bf16, f32 = jnp.bfloat16, jnp.float32
    vmem = pl.BlockSpec(memory_space=pltpu.VMEM)
    hbm = pl.BlockSpec(memory_space=pl.ANY)
    block = (cap, width)
    sem = pltpu.SemaphoreType.DMA
    return pl.pallas_call(
        functools.partial(expert_kernel, n, tps, rows, cap),
        out_shape=jax.ShapeDtypeStruct((rows, width), bf16),
        in_specs=[vmem] * 6 + [hbm] * 4,
        out_specs=vmem,
        scratch_shapes=[
            pltpu.VMEM(gated.shape, bf16),
            pltpu.VMEM(w_out.shape, bf16),
            pltpu.VMEM(w_gate.shape, bf16),
            pltpu.VMEM(w_up.shape, bf16),
            pltpu.VMEM(w_down.shape, bf16),
            pltpu.VMEM((rows, width), bf16),
            pltpu.VMEM((rows, width), bf16),
            pltpu.VMEM((n,) + block, bf16),
            pltpu.VMEM((n, tps) + block, bf16),
            pltpu.VMEM((tps,) + block, f32),
            pltpu.VMEM((2, 2) + block, f32),
            pltpu.VMEM((2,) + block, f32),
            pltpu.VMEM((n, 2) + block, bf16),
            pltpu.VMEM((n,) + block, bf16),
            pltpu.VMEM((n,) + block, bf16),
            pltpu.VMEM((n,) + block, bf16),
            pltpu.VMEM((n,) + block, bf16),
            sem((4,)), sem((tps,)), sem((tps,)),
        ] + [sem((n,))] * 12,
        compiler_params=pltpu.CompilerParams(collective_id=1, has_side_effects=True, vmem_limit_bytes=VMEM_LIMIT),
        name="experts",
    )(gated, stream, gain, place, whi, wlo, w_out, w_gate, w_up, w_down)


def slot_ranks(chosen, experts):
    onehot = (chosen[:, :, None] == jnp.arange(experts, dtype=jnp.int32)[None, None, :]).astype(
        jnp.int32
    )
    earlier = jnp.cumsum(onehot, axis=1) - onehot
    return jnp.sum(earlier * onehot, axis=2)


def per_device(
    stream,
    query,
    forget_gate_logits,
    value_input_rows,
    output_gate_logits,
    forget_floor_margin,
    additional_fading_speed,
    head_norm_gain,
    output_head_weight,
    feedforward_norm_gain,
    selected_expert_index,
    selected_expert_weight,
    expert_gate_weight,
    expert_up_weight,
    expert_down_weight,
):
    f32 = jnp.float32
    tok_rows, model_width = stream.shape
    local_scan_lanes, head_dim = forget_floor_margin.shape
    n = lax.axis_size("sp")
    tp_count = lax.axis_size("tp")
    tp_rank = lax.axis_index("tp")
    gated = gated_scan(
        n,
        query,
        forget_gate_logits,
        value_input_rows,
        output_gate_logits,
        forget_floor_margin,
        additional_fading_speed,
        head_norm_gain[None, :],
    )
    topk = selected_expert_index.shape[1]
    experts = n * expert_gate_weight.shape[0]
    group_rows = tok_rows // tp_count
    cap = 2 * topk * group_rows // experts
    cap = -(-cap // 16) * 16
    own_route = lax.dynamic_slice_in_dim(selected_expert_index, tp_rank * group_rows, group_rows, 0)
    own_stream = lax.dynamic_slice_in_dim(stream, tp_rank * group_rows, group_rows, 0)
    own_ranks = slot_ranks(own_route.reshape(1, -1), experts)[0].reshape(group_rows, topk)
    slot = own_route * cap + own_ranks
    slots = jnp.arange(experts * cap, dtype=jnp.int32)
    place = jnp.zeros((experts * cap, group_rows), f32)
    weight = jnp.zeros((group_rows, experts * cap), f32)
    for j in range(topk):
        place = place + (slot[:, j][None, :] == slots[:, None]).astype(f32)
        weight = weight + jnp.where(
            slot[:, j][:, None] == slots[None, :], selected_expert_weight[:, j][:, None], 0.0
        )
    place = place.astype(jnp.bfloat16).reshape(experts, cap, group_rows)
    weight_high = lax.reduce_precision(weight, 8, 7)
    weight_low = (weight - weight_high).astype(jnp.bfloat16)
    return experts_of(
        n,
        tp_count,
        cap,
        gated.reshape(tp_count, group_rows, local_scan_lanes * head_dim),
        own_stream,
        feedforward_norm_gain[None, :],
        place,
        weight_high.astype(jnp.bfloat16),
        weight_low,
        output_head_weight,
        expert_gate_weight[0],
        expert_up_weight[0],
        expert_down_weight[0],
    )


def solution(mesh):
    return jax.shard_map(
        per_device,
        mesh=mesh,
        in_specs=(
            P("sp", None),
            P("sp", "tp"),
            P("sp", "tp"),
            P("sp", "tp"),
            P("sp", "tp"),
            P("tp", None),
            P("sp", "tp"),
            P(),
            P(),
            P(),
            P("sp", None),
            P(("sp", "tp"), None),
            P("sp", None, "tp"),
            P("sp", None, "tp"),
            P("sp", "tp", None),
        ),
        out_specs=P(("sp", "tp"), None),
        check_vma=False,
    )
```
